32 devices in a mesh: fs: 4 (over z), tp: 4 (over y, x), rep: 2 (over core).
Axes of the slice: x: 2, y: 2, z: 4, core: 2. Of those that a mesh axis runs over, the one named last changes fastest.
Arguments:
- gate_weight: float32 [2048, 5632], P('fs', 'tp'), may hold values from -6 to 6
- gate_momentum: float32 [2048, 5632], P('fs', 'tp'), may hold values from -60 to 60
- gate_grads: float32 [2, 2048, 5632], P('rep', 'fs', 'tp'), may hold values from -3500 to 3500
- gate_rows: float32 [2048], P('fs'), may hold values from 0.3 to 3
- gate_columns: float32 [5632], P('tp'), may hold values from 0.3 to 3
- up_weight: float32 [2048, 5632], P('fs', 'tp'), may hold values from -6 to 6
- up_momentum: float32 [2048, 5632], P('fs', 'tp'), may hold values from -60 to 60
- up_grads: float32 [2, 2048, 5632], P('rep', 'fs', 'tp'), may hold values from -3500 to 3500
- up_rows: float32 [2048], P('fs'), may hold values from 0.3 to 3
- up_columns: float32 [5632], P('tp'), may hold values from 0.3 to 3
- down_weight: float32 [5632, 2048], P('fs', 'tp'), may hold values from -6 to 6
- down_momentum: float32 [5632, 2048], P('fs', 'tp'), may hold values from -60 to 60
- down_grads: float32 [2, 5632, 2048], P('rep', 'fs', 'tp'), may hold values from -3500 to 3500
- down_rows: float32 [5632], P('fs'), may hold values from 0.3 to 3
- down_columns: float32 [2048], P('tp'), may hold values from 0.3 to 3
- mixer_weight: float32 [2048, 2048], P('fs', 'tp'), may hold values from -6 to 6
- mixer_momentum: float32 [2048, 2048], P('fs', 'tp'), may hold values from -60 to 60
- mixer_grads: float32 [2, 2048, 2048], P('rep', 'fs', 'tp'), may hold values from -3500 to 3500
- mixer_rows: float32 [2048], P('fs'), may hold values from 0.3 to 3
- mixer_columns: float32 [2048], P('tp'), may hold values from 0.3 to 3
Outputs:
- gate_weight_next: float32 [2048, 5632], P('fs', 'tp')
- gate_momentum_next: float32 [2048, 5632], P('fs', 'tp')
- gate_rows_next: float32 [2048], P('fs')
- gate_columns_next: float32 [5632], P('tp')
- up_weight_next: float32 [2048, 5632], P('fs', 'tp')
- up_momentum_next: float32 [2048, 5632], P('fs', 'tp')
- up_rows_next: float32 [2048], P('fs')
- up_columns_next: float32 [5632], P('tp')
- down_weight_next: float32 [5632, 2048], P('fs', 'tp')
- down_momentum_next: float32 [5632, 2048], P('fs', 'tp')
- down_rows_next: float32 [5632], P('fs')
- down_columns_next: float32 [2048], P('tp')
- mixer_weight_next: float32 [2048, 2048], P('fs', 'tp')
- mixer_momentum_next: float32 [2048, 2048], P('fs', 'tp')
- mixer_rows_next: float32 [2048], P('fs')
- mixer_columns_next: float32 [2048], P('tp')
The draws below stay inside these ranges and needn't reach their ends.
All inputs are finite; a program needn't handle non-finite values.
Results may differ from the reference program's by a relative error of at most 0.00002.
Values sent between devices are 32-bit elements; how exact they have to be, the bound alone decides.
No kernel may reach another device: no remote copies, remote signals or barrier semaphores. Data moves between devices by JAX's collectives and lax.ppermute only.
A program may use at most 128 MiB of HBM per device.

```python
import math
import jax
import jax.numpy as jnp
from jax import lax

D = 2048
FF = 5632
N_REP = 2


def grad_draw(key, salt, height, width):
    base_key = jax.random.fold_in(key, salt)
    keys = jax.random.split(base_key, 5)
    entry_scale = 10.0 ** jax.random.uniform(keys[4], (height, width), jnp.float32, -1.0, 1.0)
    row_scale = 10.0 ** jax.random.uniform(keys[0], (height,), jnp.float32, -0.5, 0.5)
    col_scale = 10.0 ** jax.random.uniform(keys[1], (width,), jnp.float32, -0.5, 0.5)
    values = jnp.clip(jax.random.normal(keys[2], (N_REP, height, width), jnp.float32), -6.0, 6.0)
    row_trend = 3.0 ** (jnp.arange(height, dtype=jnp.float32) / height - 0.5)
    col_trend = 3.0 ** (jnp.arange(width, dtype=jnp.float32) / width - 0.5)
    scales = (row_scale * row_trend)[:, None] * (col_scale * col_trend)[None, :] * entry_scale
    return values * scales[None, :, :]


def momentum_draw(key, salt, height, width):
    base_key = jax.random.fold_in(key, salt)
    keys = jax.random.split(base_key, 2)
    entry_scale = 10.0 ** jax.random.uniform(keys[0], (height, width), jnp.float32, -1.0, 1.0)
    values = jnp.clip(jax.random.normal(keys[1], (height, width), jnp.float32), -6.0, 6.0)
    return values * entry_scale


def draw_gate_grads(key, part):
    return grad_draw(key, 11, D, FF)


def draw_up_grads(key, part):
    return grad_draw(key, 12, D, FF)


def draw_down_grads(key, part):
    return grad_draw(key, 13, FF, D)


def draw_mixer_grads(key, part):
    return grad_draw(key, 14, D, D)


def draw_gate_momentum(key, part):
    return momentum_draw(key, 21, D, FF)


def draw_up_momentum(key, part):
    return momentum_draw(key, 22, D, FF)


def draw_down_momentum(key, part):
    return momentum_draw(key, 23, FF, D)


def draw_mixer_momentum(key, part):
    return momentum_draw(key, 24, D, D)


def level_of(own_key, extent, cuts, least, largest):
    level, own = 1.0, jax.random.fold_in(own_key, 6)
    for axis_at, blocks in cuts:
        steps = jnp.exp(jax.random.uniform(jax.random.fold_in(own, axis_at), (blocks,), jnp.float32, least / len(cuts), largest / len(cuts)))
        level = level * jnp.repeat(steps, extent[axis_at] // blocks).reshape([-1 if axis == axis_at else 1 for axis in range(len(extent))])
    return level


def centred(own_key, extent, scale, most, cuts=(), held_as=jnp.bfloat16):
    loudness = level_of(own_key, extent, cuts, -0.22, 0.18) if cuts else 1.0
    entries = jax.random.normal(own_key, extent, jnp.float32) * scale * loudness
    return jnp.minimum(jnp.maximum(entries, -most), most).astype(held_as)


def setup_inputs(seed: int = 0) -> dict:
    key_of = jax.random.split(jax.random.key(seed), 21)
    gate_weight = centred(key_of[0], (D, FF), 1.0, 6.0, ((0, 4), (1, 4)), jnp.float32)
    gate_momentum = draw_gate_momentum(jax.random.fold_in(key_of[20], 71), 0)
    gate_grads = draw_gate_grads(jax.random.fold_in(key_of[20], 71), 0)
    gate_rows = jnp.clip(jnp.exp(math.log(3.0) - 2.3025851 * jax.random.uniform(key_of[3], (D,), jnp.float32) ** level_of(key_of[3], (D,), ((0, 4),), -0.2, 0.2)), 0.3, 3.0)
    gate_columns = jnp.clip(jnp.exp(math.log(3.0) - 2.3025851 * jax.random.uniform(key_of[4], (FF,), jnp.float32) ** level_of(key_of[4], (FF,), ((0, 4),), -0.2, 0.2)), 0.3, 3.0)
    up_weight = centred(key_of[5], (D, FF), 1.0, 6.0, ((0, 4), (1, 4)), jnp.float32)
    up_momentum = draw_up_momentum(jax.random.fold_in(key_of[20], 71), 0)
    up_grads = draw_up_grads(jax.random.fold_in(key_of[20], 71), 0)
    up_rows = jnp.clip(jnp.exp(math.log(3.0) - 2.3025851 * jax.random.uniform(key_of[8], (D,), jnp.float32) ** level_of(key_of[8], (D,), ((0, 4),), -0.2, 0.2)), 0.3, 3.0)
    up_columns = jnp.clip(jnp.exp(math.log(3.0) - 2.3025851 * jax.random.uniform(key_of[9], (FF,), jnp.float32) ** level_of(key_of[9], (FF,), ((0, 4),), -0.2, 0.2)), 0.3, 3.0)
    down_weight = centred(key_of[10], (FF, D), 1.0, 6.0, ((0, 4), (1, 4)), jnp.float32)
    down_momentum = draw_down_momentum(jax.random.fold_in(key_of[20], 71), 0)
    down_grads = draw_down_grads(jax.random.fold_in(key_of[20], 71), 0)
    down_rows = jnp.clip(jnp.exp(math.log(3.0) - 2.3025851 * jax.random.uniform(key_of[13], (FF,), jnp.float32) ** level_of(key_of[13], (FF,), ((0, 4),), -0.2, 0.2)), 0.3, 3.0)
    down_columns = jnp.clip(jnp.exp(math.log(3.0) - 2.3025851 * jax.random.uniform(key_of[14], (D,), jnp.float32) ** level_of(key_of[14], (D,), ((0, 4),), -0.2, 0.2)), 0.3, 3.0)
    mixer_weight = centred(key_of[15], (D, D), 1.0, 6.0, ((0, 4), (1, 4)), jnp.float32)
    mixer_momentum = draw_mixer_momentum(jax.random.fold_in(key_of[20], 71), 0)
    mixer_grads = draw_mixer_grads(jax.random.fold_in(key_of[20], 71), 0)
    mixer_rows = jnp.clip(jnp.exp(math.log(3.0) - 2.3025851 * jax.random.uniform(key_of[18], (D,), jnp.float32) ** level_of(key_of[18], (D,), ((0, 4),), -0.2, 0.2)), 0.3, 3.0)
    mixer_columns = jnp.clip(jnp.exp(math.log(3.0) - 2.3025851 * jax.random.uniform(key_of[19], (D,), jnp.float32) ** level_of(key_of[19], (D,), ((0, 4),), -0.2, 0.2)), 0.3, 3.0)
    return {"gate_weight": gate_weight, "gate_momentum": gate_momentum, "gate_grads": gate_grads, "gate_rows": gate_rows, "gate_columns": gate_columns, "up_weight": up_weight, "up_momentum": up_momentum, "up_grads": up_grads, "up_rows": up_rows, "up_columns": up_columns, "down_weight": down_weight, "down_momentum": down_momentum, "down_grads": down_grads, "down_rows": down_rows, "down_columns": down_columns, "mixer_weight": mixer_weight, "mixer_momentum": mixer_momentum, "mixer_grads": mixer_grads, "mixer_rows": mixer_rows, "mixer_columns": mixer_columns}


momentum_decay = 0.9
moment_decay = 0.95
clip_level = 0.25
step_rate = 0.1

def update_matrix(weight, momentum, grads, rows, columns):
    grad = lax.optimization_barrier(jnp.sum(grads.astype(jnp.float32), axis=0))
    momentum_next = momentum_decay * momentum + (1.0 - momentum_decay) * grad
    squares = grad * grad
    rows_next = moment_decay * rows + (1.0 - moment_decay) * lax.optimization_barrier(jnp.mean(squares, axis=1))
    columns_next = moment_decay * columns + (1.0 - moment_decay) * lax.optimization_barrier(jnp.mean(squares, axis=0))
    row_mean = jnp.mean(rows_next)
    update = momentum_next * lax.rsqrt(rows_next[:, None] * columns_next[None, :] / row_mean)
    spread = jnp.sqrt(jnp.mean(update * update))
    factor = jnp.maximum(1.0, spread / clip_level)
    weight_next = weight - step_rate * update / factor
    return (weight_next, momentum_next, rows_next, columns_next)

def reference(gate_weight, gate_momentum, gate_grads, gate_rows, gate_columns, up_weight, up_momentum, up_grads, up_rows, up_columns, down_weight, down_momentum, down_grads, down_rows, down_columns, mixer_weight, mixer_momentum, mixer_grads, mixer_rows, mixer_columns):
    first = update_matrix(gate_weight, gate_momentum, gate_grads, gate_rows, gate_columns)
    second = update_matrix(up_weight, up_momentum, up_grads, up_rows, up_columns)
    third = update_matrix(down_weight, down_momentum, down_grads, down_rows, down_columns)
    fourth = update_matrix(mixer_weight, mixer_momentum, mixer_grads, mixer_rows, mixer_columns)
    return (first[0], first[1], first[2], first[3], second[0], second[1], second[2], second[3], third[0], third[1], third[2], third[3], fourth[0], fourth[1], fourth[2], fourth[3])
```

```python
import jax
import jax.numpy as jnp
from jax import lax
from jax.sharding import PartitionSpec as P

momentum_decay = 0.9
moment_decay = 0.95
clip_level = 0.25
step_rate = 0.1

EVERY = ("fs", "tp", "rep")
SWAP = [(0, 1), (1, 0)]
ORDER = (3, 0, 1, 2)


def swap(x):
    return lax.ppermute(x, "rep", SWAP)


def half(x, which):
    size = x.shape[0] // 2
    return lax.dynamic_slice_in_dim(x, which * size, size, 0)


def join(own, other, me):
    first = me == 0
    return jnp.concatenate([jnp.where(first, own, other), jnp.where(first, other, own)], axis=0)


def cross_sums(row_part, column_part, me):
    n_fs, n_tp = lax.axis_size("fs"), lax.axis_size("tp")
    if n_fs != n_tp:
        return lax.psum(row_part, "tp"), lax.psum(column_part, "fs")
    length = max(row_part.size, column_part.size)

    def padded(x):
        return jnp.pad(x, (0, length - x.size))

    mine = jnp.where(me == 1, padded(row_part), padded(column_part))
    total = mine
    for shift in range(1, n_tp):
        pairs = []
        for f in range(n_fs):
            for t in range(n_tp):
                here = (f * n_tp + t) * 2
                pairs.append((here + 1, (f * n_tp + (t + shift) % n_tp) * 2 + 1))
                pairs.append((here, ((f + shift) % n_fs * n_tp + t) * 2))
        total = total + lax.ppermute(mine, EVERY, pairs)
    other = swap(total)
    rows = jnp.where(me == 1, total, other)[: row_part.size]
    columns = jnp.where(me == 1, other, total)[: column_part.size]
    return rows, columns


def body(*args):
    weights, momenta, partials, rows, columns = (args[k::5] for k in range(5))
    me = lax.axis_index("rep")
    n_all = lax.axis_size(EVERY)
    partials = [item[0] for item in partials]
    heights = [item.shape[0] for item in weights]
    widths = [item.shape[1] for item in weights]
    row_count = [h * lax.axis_size("fs") for h in heights]
    column_count = [w * lax.axis_size("tp") for w in widths]

    received = [None] * 4
    for k in ORDER:
        received[k] = swap(half(partials[k], 1 - me))
    own = [None] * 4
    back = [None] * 4
    row_local = [None] * 4
    column_local = [None] * 4
    for k in ORDER:
        grad = half(partials[k], me) + received[k]
        own[k] = momentum_decay * half(momenta[k], me) + (1.0 - momentum_decay) * grad
        back[k] = swap(own[k])
        square = grad * grad
        placed = jnp.zeros((heights[k],), jnp.float32)
        row_local[k] = lax.dynamic_update_slice_in_dim(
            placed, jnp.sum(square, axis=1), me * (heights[k] // 2), 0
        )
        column_local[k] = jnp.sum(square, axis=0)

    local = jnp.concatenate(row_local + column_local)
    local = local + swap(local)
    n_rows = sum(heights)
    row_total, column_total = cross_sums(local[:n_rows], local[n_rows:], me)

    rows_next, columns_next = [], []
    at_row = at_column = 0
    for k in range(4):
        r = row_total[at_row : at_row + heights[k]]
        c = column_total[at_column : at_column + widths[k]]
        at_row += heights[k]
        at_column += widths[k]
        rows_next.append(moment_decay * rows[k] + (1.0 - moment_decay) * r / column_count[k])
        columns_next.append(moment_decay * columns[k] + (1.0 - moment_decay) * c / row_count[k])

    mass = []
    for k in range(4):
        m = own[k]
        mass.append(jnp.sum(m * m / half(rows_next[k], me)[:, None] / columns_next[k][None, :]))
    row_mass = [jnp.sum(half(rows_next[k], me)) for k in range(4)]
    scalars = jnp.stack(mass + row_mass)
    spread_out = jnp.broadcast_to(scalars[None], (n_all, 8))
    totals = jnp.sum(lax.all_to_all(spread_out, EVERY, 0, 0), axis=0)

    weights_next, momenta_next = [], []
    for k in range(4):
        row_mean = totals[4 + k] / (lax.axis_size("tp") * row_count[k])
        spread = jnp.sqrt(totals[k] * row_mean / (row_count[k] * column_count[k]))
        factor = jnp.maximum(1.0, spread / clip_level)
        scale = step_rate * jnp.sqrt(row_mean) / factor
        m = join(own[k], back[k], me)
        momenta_next.append(m)
        by_row = lax.rsqrt(rows_next[k]) * scale
        by_column = lax.rsqrt(columns_next[k])
        weights_next.append(weights[k] - m * by_row[:, None] * by_column[None, :])
    out = []
    for k in range(4):
        out += [weights_next[k], momenta_next[k], rows_next[k], columns_next[k]]
    return tuple(out)


def solution(mesh):
    matrix, stacked = P("fs", "tp"), P("rep", "fs", "tp")
    return jax.shard_map(
        body,
        mesh=mesh,
        in_specs=(matrix, matrix, stacked, P("fs"), P("tp")) * 4,
        out_specs=(matrix, matrix, P("fs"), P("tp")) * 4,
        check_vma=False,
    )
```

```python
import jax
import jax.numpy as jnp
from jax import lax
from jax.experimental import pallas as pl
from jax.experimental.pallas import tpu as pltpu
from jax.sharding import PartitionSpec as P


momentum_decay = 0.9
moment_decay = 0.95
clip_level = 0.25
step_rate = 0.1

EVERY = ("fs", "tp", "rep")
SWAP = [(0, 1), (1, 0)]
ORDER = (0, 1, 2, 3)
LANES = 128
PARTS = 2
HBM = pl.BlockSpec(memory_space=pltpu.HBM)
VMEM = pl.BlockSpec(memory_space=pltpu.VMEM)


def up_to(n, unit):
    return (n + unit - 1) // unit * unit


def struct(*shape):
    return jax.ShapeDtypeStruct(shape, jnp.float32)


def call(kernel, ins, outs, spaces, out_spaces, scratch=(), limit=4 << 20, cost=0, aliases=None):
    ins = [pltpu.with_memory_space_constraint(x, spec.memory_space) for x, spec in zip(ins, spaces)]
    placed = [spec.memory_space(out.shape, out.dtype) for out, spec in zip(outs, out_spaces)]
    return pl.pallas_call(
        kernel,
        out_shape=placed,
        in_specs=spaces,
        out_specs=out_spaces,
        scratch_shapes=scratch,
        input_output_aliases=aliases or {},
        compiler_params=pltpu.CompilerParams(vmem_limit_bytes=limit),
        cost_estimate=pl.CostEstimate(flops=cost, bytes_accessed=0, transcendentals=0),
    )(*ins)


def swap(x):
    return lax.ppermute(x, "rep", SWAP)


def copies(pairs, sem):
    started = [pltpu.make_async_copy(a, b, sem.at[n]) for n, (a, b) in enumerate(pairs)]
    for item in started:
        item.start()
    for item in started:
        item.wait()


def other_halves(arrays):
    n = len(arrays)

    def kernel(*refs):
        me = lax.axis_index("rep")
        pairs = []
        for source, target in zip(refs[:n], refs[n : 2 * n]):
            h = target.shape[0]
            pairs.append((source.at[0, pl.ds(pl.multiple_of((1 - me) * h, 8), h)], target))
        copies(pairs, refs[-1])

    outs = [struct(g.shape[1] // 2, g.shape[2]) for g in arrays]
    return call(kernel, arrays, outs, [HBM] * n, [VMEM] * n, [pltpu.SemaphoreType.DMA((n,))], cost=1 << 21)


def own_halves(arrays):
    n = len(arrays)

    def kernel(*refs):
        me = lax.axis_index("rep")
        sem = refs[-1]
        pairs = []
        for source, target in zip(refs[:n], refs[n : 2 * n]):
            h = target.shape[0]
            at = pl.ds(pl.multiple_of(me * h, 8), h)
            pairs.append((source.at[0, at] if len(source.shape) == 3 else source.at[at], target))
        copies(pairs, sem)

    outs = [struct(a.shape[-2] // 2, a.shape[-1]) for a in arrays]
    return call(kernel, arrays, outs, [HBM] * n, [VMEM] * n, [pltpu.SemaphoreType.DMA((n,))], cost=1 << 22)


class Places:
    def __init__(self, heights, widths):
        self.halves = [h // 2 for h in heights]
        self.blocks = [up_to(h, LANES) // LANES for h in self.halves]
        self.tiles = [w // LANES for w in widths]
        self.row_at = [sum(self.blocks[:k]) for k in range(4)]
        self.column_at = [sum(self.tiles[:k]) for k in range(4)]
        self.n_row = up_to(sum(self.blocks), 8)
        self.spare = sum(self.tiles)
        self.n_column = up_to(self.spare + 1, 8)


def statistics(k, places, g, m, received, packed):
    h, width = g.shape
    n_blocks, tiles = places.blocks[k], places.tiles[k]
    row_at, column_at = places.row_at[k], places.n_row + places.column_at[k]

    def kernel(*refs):
        g_ref, m_ref, r_ref = refs[:3]
        own_ref, out_ref, partial = refs[-3:]
        if packed is None:
            out_ref[...] = jnp.zeros_like(out_ref)

        def step(i, sums):
            rows = pl.ds(pl.multiple_of(i * 8, 8), 8)
            sums = list(sums)
            by_row = None
            for j in range(tiles):
                at = (rows, pl.ds(j * LANES, LANES))
                grad = g_ref[at] + r_ref[at]
                own_ref[at] = momentum_decay * m_ref[at] + (1.0 - momentum_decay) * grad
                square = grad * grad
                sums[j] = sums[j] + square
                by_row = square if by_row is None else by_row + square
            partial[rows, :] = by_row
            return tuple(sums)

        zero = jnp.zeros((8, LANES), jnp.float32)
        sums = lax.fori_loop(0, h // 8, step, (zero,) * tiles, unroll=2)
        for j in range(tiles):
            out_ref[pl.ds(column_at + j, 1), :] = jnp.sum(sums[j], axis=0, keepdims=True)
        if n_blocks * LANES > h:
            partial[pl.ds(h, n_blocks * LANES - h), :] = jnp.zeros((n_blocks * LANES - h, LANES), jnp.float32)
        for b in range(n_blocks):
            turned = partial[pl.ds(b * LANES, LANES), :].T
            out_ref[pl.ds(row_at + b, 1), :] = jnp.sum(turned, axis=0, keepdims=True)

    ins = [g, m, received] + ([] if packed is None else [packed])
    return call(
        kernel,
        ins,
        [struct(h, width), struct(places.n_row + places.n_column, LANES)],
        [VMEM] * len(ins),
        [VMEM, VMEM],
        [pltpu.VMEM((n_blocks * LANES, LANES), jnp.float32)],
        cost=1 << 20,
        aliases=None if packed is None else {3: 1},
    )


def spread_rows(root, factor, n_blocks):
    for b in range(n_blocks):
        wide = jnp.broadcast_to(root[b : b + 1, :], (LANES, LANES)).T
        factor[pl.ds(b * LANES, LANES), :] = wide


def shares(places, column_count, rows_old, row_parts, packed, own, after):
    n_parts = len(row_parts)

    def old_rows(k, ref, me):
        h, n = places.halves[k], places.blocks[k]
        whole, rest = divmod(h, LANES)
        everything = ref[...]
        first = everything[:n]
        if rest:
            turned = pltpu.roll(everything, LANES - rest, 1)
            low = lax.broadcasted_iota(jnp.int32, (1, LANES), 1) < LANES - rest
            steps = []
            for i in range(n):
                here = turned[whole + i : whole + i + 1]
                after = turned[whole + i + 1 : whole + i + 2] if i < n - 1 else here
                steps.append(jnp.where(low, here, after))
            second = jnp.concatenate(steps, axis=0)
            at = lax.broadcasted_iota(jnp.int32, (n, LANES), 0) * LANES + lax.broadcasted_iota(jnp.int32, (n, LANES), 1)
            return jnp.where(at < h, jnp.where(me == 0, first, second), 0.0)
        return jnp.where(me == 0, first, everything[n:])

    def kernel(*refs):
        rows_refs, packed_ref = refs[:4], refs[4]
        part_refs, own_refs = refs[5 : 5 + n_parts], refs[5 + n_parts : 9 + n_parts]
        rows_out, factor, out_ref = refs[-3:]
        lane = lax.broadcasted_iota(jnp.int32, (1, LANES), 1)
        total = packed_ref[pl.ds(0, places.n_row), :]
        for part in part_refs:
            total = total + part[...]
        me = lax.axis_index("rep")
        mass = jnp.zeros((1, LANES), jnp.float32)
        out_ref[pl.ds(0, places.n_column), :] = packed_ref[pl.ds(places.n_row, places.n_column), :]
        out_ref[pl.ds(2 * places.n_column - 8, 8), :] = jnp.zeros((8, LANES), jnp.float32)
        news = []
        for k in range(4):
            at = slice(places.row_at[k], places.row_at[k] + places.blocks[k])
            r = moment_decay * old_rows(k, rows_refs[k], me) + (1.0 - moment_decay) / column_count[k] * total[at, :]
            news.append(r)
            mass = jnp.where(lane == k, jnp.sum(r), mass)
            rows_out[pl.ds(places.row_at[k], places.blocks[k]), :] = r
        fill = places.n_row - sum(places.blocks)
        if fill:
            rows_out[pl.ds(sum(places.blocks), fill), :] = jnp.ones((fill, LANES), jnp.float32)
        spread_rows(lax.rsqrt(jnp.concatenate(news, axis=0)), factor, sum(places.blocks))
        for k, m_ref in enumerate(own_refs):
            first = places.row_at[k] * LANES

            def step(i, sums):
                sums = list(sums)
                by_row = factor[pl.ds(pl.multiple_of(first + i * 8, 8), 8), :]
                for j in range(places.tiles[k]):
                    v = m_ref[pl.ds(pl.multiple_of(i * 8, 8), 8), pl.ds(j * LANES, LANES)] * by_row
                    sums[j] = sums[j] + v * v
                return tuple(sums)

            zero = jnp.zeros((8, LANES), jnp.float32)
            sums = lax.fori_loop(0, places.halves[k] // 8, step, (zero,) * places.tiles[k], unroll=2)
            for j in range(places.tiles[k]):
                at = pl.ds(places.n_column + places.column_at[k] + j, 1)
                out_ref[at, :] = jnp.sum(sums[j], axis=0, keepdims=True)
        out_ref[pl.ds(places.n_column + places.spare, 1), :] = mass

    return call(
        kernel,
        [*rows_old, packed, *row_parts, *own, *after],
        [struct(places.n_row, LANES), struct(sum(places.blocks) * LANES, LANES), struct(2 * places.n_column, LANES)],
        [VMEM] * (9 + n_parts) + [HBM] * len(after),
        [VMEM] * 3,
        cost=1 << 21,
    )


def columns(places, row_count, columns_old, total, other, after):
    def kernel(c0, c1, c2, c3, total_ref, other_ref, *rest):
        columns_out, out_ref = rest[-2:]
        old_refs = (c0, c1, c2, c3)
        lane = lax.broadcasted_iota(jnp.int32, (1, LANES), 1)
        both = total_ref[...] + other_ref[...]
        mass = jnp.zeros((1, LANES), jnp.float32)
        columns_out[pl.ds(places.n_column - 8, 8), :] = jnp.zeros((8, LANES), jnp.float32)
        row_mass = both[places.n_column + places.spare : places.n_column + places.spare + 1, :]
        for k in range(4):
            at = slice(places.column_at[k], places.column_at[k] + places.tiles[k])
            c = moment_decay * old_refs[k][...] + (1.0 - moment_decay) / row_count[k] * both[at, :]
            columns_out[pl.ds(places.column_at[k], places.tiles[k]), :] = c
            at = slice(places.n_column + at.start, places.n_column + at.stop)
            mass = jnp.where(lane == k, jnp.sum(both[at, :] / c), mass)
            mass = jnp.where(lane == 4 + k, jnp.sum(jnp.where(lane == k, row_mass, 0.0)), mass)
        out_ref[...] = jnp.broadcast_to(mass, (8, LANES))

    return call(
        kernel,
        [*columns_old, total, other, *after],
        [struct(places.n_column, LANES), struct(8, LANES)],
        [VMEM] * 6 + [HBM] * len(after),
        [VMEM] * 2,
        cost=1 << 20,
    )


def load_weights(weights, after):
    n = len(weights)

    def kernel(*refs):
        copies(list(zip(refs[:n], refs[n + 1 : 2 * n + 1])), refs[-1])

    return call(
        kernel,
        [*weights, after],
        [struct(*w.shape) for w in weights],
        [HBM] * n + [VMEM],
        [VMEM] * n,
        [pltpu.SemaphoreType.DMA((n,))],
        cost=1 << 24,
    )


def write_own(own, shapes, weights, after):
    n = len(weights)

    def kernel(*refs):
        me = lax.axis_index("rep")
        outs = refs[5 + n :]
        pairs = list(zip(refs[5 : 5 + n], outs[4 : 4 + n]))
        for k in range(4):
            h = refs[k].shape[0]
            pairs.append((refs[k], outs[k].at[pl.ds(pl.multiple_of(me * h, 8), h)]))
        copies(pairs, refs[-1])

    out = call(
        kernel,
        [*own, after, *weights],
        shapes + [struct(*w.shape) for w in weights],
        [VMEM] * 5 + [HBM] * n,
        [HBM] * 4 + [VMEM] * n,
        [pltpu.SemaphoreType.DMA((4 + n,))],
        cost=1 << 24,
    )
    return out[:4], out[4:]


def write_back(back, momenta):
    def kernel(*refs):
        me = lax.axis_index("rep")
        pairs = []
        for k in range(4):
            h = refs[k].shape[0]
            pairs.append((refs[k], refs[8 + k].at[pl.ds(pl.multiple_of((1 - me) * h, 8), h)]))
        copies(pairs, refs[-1])

    return call(
        kernel,
        [*back, *momenta],
        [struct(*m.shape) for m in momenta],
        [VMEM] * 4 + [HBM] * 4,
        [HBM] * 4,
        [pltpu.SemaphoreType.DMA((4,))],
        cost=1 << 24,
        aliases={4 + k: k for k in range(4)},
    )


def write_moments(places, rows_own, rows_other, columns_new):
    counts = [2 * h // LANES for h in places.halves]

    def kernel(own_ref, other_ref, columns_ref, *outs):
        me = lax.axis_index("rep")
        row_refs, column_refs = outs[:4], outs[4:8]
        spread_rows(lax.rsqrt(other_ref[...]), outs[8], sum(places.blocks))
        for k in range(4):
            h, n = places.halves[k], places.blocks[k]
            column_refs[k][...] = columns_ref[pl.ds(places.column_at[k], places.tiles[k]), :]
            mine = own_ref[pl.ds(places.row_at[k], n), :]
            other = other_ref[pl.ds(places.row_at[k], n), :]
            first = jnp.where(me == 0, mine, other)
            second = jnp.where(me == 0, other, mine)
            whole, rest = divmod(h, LANES)
            if not rest:
                row_refs[k][pl.ds(0, n), :] = first
                row_refs[k][pl.ds(n, n), :] = second
                continue
            turned = pltpu.roll(second, rest, 1)
            low = lax.broadcasted_iota(jnp.int32, (1, LANES), 1) < rest
            row_refs[k][pl.ds(0, whole), :] = first[:whole]
            before = first[whole : whole + 1]
            for i in range(counts[k] - whole):
                here = turned[i : i + 1]
                row_refs[k][pl.ds(whole + i, 1), :] = jnp.where(low, before, here)
                before = here

    ins = [pltpu.with_memory_space_constraint(x, pltpu.VMEM) for x in (rows_own, rows_other, columns_new)]
    out = pl.pallas_call(
        kernel,
        name="write_moments",
        out_shape=[struct(n, LANES) for n in counts + places.tiles]
        + [pltpu.VMEM((sum(places.blocks) * LANES, LANES), jnp.float32)],
        in_specs=[VMEM] * 3,
        out_specs=[VMEM] * 9,
        compiler_params=pltpu.CompilerParams(vmem_limit_bytes=2 << 20),
        cost_estimate=pl.CostEstimate(flops=1 << 24, bytes_accessed=0, transcendentals=0),
    )(*ins)
    return out[:4], out[4:8], out[8]


def write_weights(places, row_count, column_count, n_share, masses, factors, columns_new, own, back, weights, outs):
    n_parts = len(masses)

    def kernel(*refs):
        part_refs, refs = refs[:n_parts], refs[n_parts:]
        factor_refs, columns_ref = refs[:2], refs[2]
        own_refs, back_refs, w_refs, out_refs = (refs[3 + 4 * n : 7 + 4 * n] for n in range(4))
        stages, sem = refs[19:23], refs[23]
        me = lax.axis_index("rep")
        masses_all = sum((part[pl.ds(0, 1), :] for part in part_refs[1:]), part_refs[0][pl.ds(0, 1), :])
        lane = lax.broadcasted_iota(jnp.int32, (1, LANES), 1)

        def pick(n):
            return jnp.sum(jnp.where(lane == n, masses_all, 0.0), axis=1, keepdims=True)

        waits = []
        for k in range(4):
            h, tiles = places.halves[k], places.tiles[k]
            row_mean = pick(4 + k) / (n_share * row_count[k])
            spread = jnp.sqrt(pick(k) * row_mean / (row_count[k] * column_count[k]))
            scale = step_rate * jnp.sqrt(row_mean) / jnp.maximum(1.0, spread / clip_level)
            by_column = lax.rsqrt(columns_ref[pl.ds(places.column_at[k], tiles), :]) * scale
            wide = [jnp.broadcast_to(by_column[j : j + 1, :], (8, LANES)) for j in range(tiles)]
            chunk = h // PARTS if h % (8 * PARTS) == 0 else h
            first = places.row_at[k] * LANES
            for side, m_ref in enumerate((own_refs[k], back_refs[k])):
                which = me if side == 0 else 1 - me
                factor_ref = factor_refs[side]
                for begin in range(0, h, chunk):

                    def step(i, carry):
                        near = pl.multiple_of(begin + i * 8, 8)
                        far = pl.multiple_of(which * h + begin + i * 8, 8)
                        by_row = factor_ref[pl.ds(pl.multiple_of(first + begin + i * 8, 8), 8), :]
                        for j in range(tiles):
                            lanes = pl.ds(j * LANES, LANES)
                            change = m_ref[pl.ds(near, 8), lanes] * by_row * wide[j]
                            stages[k][pl.ds(far, 8), lanes] = w_refs[k][pl.ds(far, 8), lanes] - change
                        return carry

                    lax.fori_loop(0, chunk // 8, step, 0, unroll=2)
                    at = pl.ds(pl.multiple_of(which * h + begin, 8), chunk)
                    copy = pltpu.make_async_copy(stages[k].at[at], out_refs[k].at[at], sem.at[len(waits)])
                    copy.start()
                    waits.append(copy)
        for copy in waits:
            copy.wait()

    scratch = [pltpu.VMEM(w.shape, jnp.float32) for w in weights] + [pltpu.SemaphoreType.DMA((8 * PARTS,))]
    limit = sum(w.size * 4 for w in weights) + (4 << 20)
    return call(
        kernel,
        [*masses, *factors, columns_new, *own, *back, *weights],
        outs,
        [VMEM] * (n_parts + 15),
        [HBM] * 4,
        scratch,
        limit=limit,
        cost=1 << 22,
    )


def shifted(x, axis):
    n = lax.axis_size(axis)
    out = []
    for d in range(1, n):
        if n & (n - 1):
            pairs = [(i, (i + d) % n) for i in range(n)]
        else:
            pairs = [(i, i ^ d) for i in range(n)]
        out.append(lax.ppermute(x, axis, pairs))
    return out


def fast_body(*args):
    weights, momenta, partials, rows, columns_in = (args[k::5] for k in range(5))
    n_fs, n_tp = lax.axis_size("fs"), lax.axis_size("tp")
    heights = [item.shape[0] for item in weights]
    widths = [item.shape[1] for item in weights]
    row_count = [h * n_fs for h in heights]
    column_count = [w * n_tp for w in widths]
    places = Places(heights, widths)
    shapes = [struct(*w.shape) for w in weights]

    received = [None] * 4
    for group in (ORDER[:1], ORDER[1:]):
        for k, other in zip(group, other_halves([partials[k] for k in group])):
            received[k] = swap(other)
    halves = own_halves([*partials, *momenta])
    rows_old = [item.reshape(-1, LANES) for item in rows]
    columns_old = [item.reshape(-1, LANES) for item in columns_in]
    own, back, packed = [None] * 4, [None] * 4, None
    for k in ORDER:
        own[k], packed = statistics(k, places, halves[k], halves[4 + k], received[k], packed)
        back[k] = swap(own[k])

    row_parts = shifted(packed[: places.n_row], "tp")
    held_first = load_weights([weights[0], weights[3]], packed)
    rows_own, factor_own, local = shares(places, column_count, rows_old, row_parts, packed, own, ())

    rows_other = swap(rows_own)
    total = sum(shifted(local, "fs"), local)
    momenta_next, held_second = write_own(own, shapes, [weights[1], weights[2]], local)
    momenta_next = write_back(back, momenta_next)
    columns_new, mass = columns(places, row_count, columns_old, total, swap(total), ())

    held = [held_first[0], *held_second, held_first[1]]
    masses = [mass, *shifted(mass, "tp")]
    rows_new, columns_out, factor_other = write_moments(places, rows_own, rows_other, columns_new)
    weights_next = write_weights(
        places, row_count, column_count, n_tp, masses, [factor_own, factor_other], columns_new, own, back, held, shapes
    )
    out = []
    for k in range(4):
        out += [weights_next[k], momenta_next[k], rows_new[k].reshape(-1), columns_out[k].reshape(-1)]
    return tuple(out)


def half(x, which):
    size = x.shape[0] // 2
    return lax.dynamic_slice_in_dim(x, which * size, size, 0)


def join(own, other, me):
    first = me == 0
    return jnp.concatenate([jnp.where(first, own, other), jnp.where(first, other, own)], axis=0)


def cross_sums(row_part, column_part, me):
    n_fs, n_tp = lax.axis_size("fs"), lax.axis_size("tp")
    if n_fs != n_tp:
        return lax.psum(row_part, "tp"), lax.psum(column_part, "fs")
    length = max(row_part.size, column_part.size)

    def padded(x):
        return jnp.pad(x, (0, length - x.size))

    mine = jnp.where(me == 1, padded(row_part), padded(column_part))
    total = mine
    for shift in range(1, n_tp):
        pairs = []
        for f in range(n_fs):
            for t in range(n_tp):
                here = (f * n_tp + t) * 2
                pairs.append((here + 1, (f * n_tp + (t + shift) % n_tp) * 2 + 1))
                pairs.append((here, ((f + shift) % n_fs * n_tp + t) * 2))
        total = total + lax.ppermute(mine, EVERY, pairs)
    other = swap(total)
    rows = jnp.where(me == 1, total, other)[: row_part.size]
    columns = jnp.where(me == 1, other, total)[: column_part.size]
    return rows, columns


def plain_body(*args):
    weights, momenta, partials, rows, columns = (args[k::5] for k in range(5))
    me = lax.axis_index("rep")
    n_all = lax.axis_size(EVERY)
    partials = [item[0] for item in partials]
    heights = [item.shape[0] for item in weights]
    widths = [item.shape[1] for item in weights]
    row_count = [h * lax.axis_size("fs") for h in heights]
    column_count = [w * lax.axis_size("tp") for w in widths]

    received = [None] * 4
    for k in ORDER:
        received[k] = swap(half(partials[k], 1 - me))
    own = [None] * 4
    back = [None] * 4
    row_local = [None] * 4
    column_local = [None] * 4
    for k in ORDER:
        grad = half(partials[k], me) + received[k]
        own[k] = momentum_decay * half(momenta[k], me) + (1.0 - momentum_decay) * grad
        back[k] = swap(own[k])
        square = grad * grad
        placed = jnp.zeros((heights[k],), jnp.float32)
        row_local[k] = lax.dynamic_update_slice_in_dim(
            placed, jnp.sum(square, axis=1), me * (heights[k] // 2), 0
        )
        column_local[k] = jnp.sum(square, axis=0)

    local = jnp.concatenate(row_local + column_local)
    local = local + swap(local)
    n_rows = sum(heights)
    row_total, column_total = cross_sums(local[:n_rows], local[n_rows:], me)

    rows_next, columns_next = [], []
    at_row = at_column = 0
    for k in range(4):
        r = row_total[at_row : at_row + heights[k]]
        c = column_total[at_column : at_column + widths[k]]
        at_row += heights[k]
        at_column += widths[k]
        rows_next.append(moment_decay * rows[k] + (1.0 - moment_decay) * r / column_count[k])
        columns_next.append(moment_decay * columns[k] + (1.0 - moment_decay) * c / row_count[k])

    mass = []
    for k in range(4):
        m = own[k]
        mass.append(jnp.sum(m * m / half(rows_next[k], me)[:, None] / columns_next[k][None, :]))
    row_mass = [jnp.sum(half(rows_next[k], me)) for k in range(4)]
    scalars = jnp.stack(mass + row_mass)
    spread_out = jnp.broadcast_to(scalars[None], (n_all, 8))
    totals = jnp.sum(lax.all_to_all(spread_out, EVERY, 0, 0), axis=0)

    weights_next, momenta_next = [], []
    for k in range(4):
        row_mean = totals[4 + k] / (lax.axis_size("tp") * row_count[k])
        spread = jnp.sqrt(totals[k] * row_mean / (row_count[k] * column_count[k]))
        factor = jnp.maximum(1.0, spread / clip_level)
        scale = step_rate * jnp.sqrt(row_mean) / factor
        m = join(own[k], back[k], me)
        momenta_next.append(m)
        by_row = lax.rsqrt(rows_next[k]) * scale
        by_column = lax.rsqrt(columns_next[k])
        weights_next.append(weights[k] - m * by_row[:, None] * by_column[None, :])
    out = []
    for k in range(4):
        out += [weights_next[k], momenta_next[k], rows_next[k], columns_next[k]]
    return tuple(out)


def fits(args):
    small = max(lax.axis_size("fs"), lax.axis_size("tp")) <= 8
    return small and all(n % LANES == 0 for item in args[0::5] for n in item.shape)


def body(*args):
    return fast_body(*args) if fits(args) else plain_body(*args)


def solution(mesh):
    matrix, stacked = P("fs", "tp"), P("rep", "fs", "tp")

    return jax.shard_map(
        body,
        mesh=mesh,
        in_specs=(matrix, matrix, stacked, P("fs"), P("tp")) * 4,
        out_specs=(matrix, matrix, P("fs"), P("tp")) * 4,
        check_vma=False,
    )
```

```python
import jax
import jax.numpy as jnp
from jax import lax
from jax.experimental import pallas as pl
from jax.experimental.pallas import tpu as pltpu
from jax.sharding import PartitionSpec as P


momentum_decay = 0.9
moment_decay = 0.95
clip_level = 0.25
step_rate = 0.1

EVERY = ("fs", "tp", "rep")
SWAP = [(0, 1), (1, 0)]
ORDER = (0, 1, 2, 3)
LANES = 128
PARTS = 2
HBM = pl.BlockSpec(memory_space=pltpu.HBM)
VMEM = pl.BlockSpec(memory_space=pltpu.VMEM)


def up_to(n, unit):
    return (n + unit - 1) // unit * unit


def struct(*shape):
    return jax.ShapeDtypeStruct(shape, jnp.float32)


def call(kernel, ins, outs, spaces, out_spaces, scratch=(), limit=4 << 20, cost=0, aliases=None):
    ins = [pltpu.with_memory_space_constraint(x, spec.memory_space) for x, spec in zip(ins, spaces)]
    placed = [spec.memory_space(out.shape, out.dtype) for out, spec in zip(outs, out_spaces)]
    return pl.pallas_call(
        kernel,
        out_shape=placed,
        in_specs=spaces,
        out_specs=out_spaces,
        scratch_shapes=scratch,
        input_output_aliases=aliases or {},
        compiler_params=pltpu.CompilerParams(vmem_limit_bytes=limit),
        cost_estimate=pl.CostEstimate(flops=cost, bytes_accessed=0, transcendentals=0),
    )(*ins)


def swap(x):
    return lax.ppermute(x, "rep", SWAP)


def copies(pairs, sem):
    started = [pltpu.make_async_copy(a, b, sem.at[n]) for n, (a, b) in enumerate(pairs)]
    for item in started:
        item.start()
    for item in started:
        item.wait()


def other_halves(arrays):
    n = len(arrays)

    def kernel(*refs):
        me = lax.axis_index("rep")
        pairs = []
        for source, target in zip(refs[:n], refs[n : 2 * n]):
            h = target.shape[0]
            pairs.append((source.at[0, pl.ds(pl.multiple_of((1 - me) * h, 8), h)], target))
        copies(pairs, refs[-1])

    outs = [struct(g.shape[1] // 2, g.shape[2]) for g in arrays]
    return call(kernel, arrays, outs, [HBM] * n, [VMEM] * n, [pltpu.SemaphoreType.DMA((n,))], cost=1 << 21)


class Places:
    def __init__(self, heights, widths):
        self.halves = [h // 2 for h in heights]
        self.widths = widths
        self.blocks = [up_to(h, LANES) // LANES for h in self.halves]
        self.tiles = [w // LANES for w in widths]
        self.row_at = [sum(self.blocks[:k]) for k in range(4)]
        self.column_at = [sum(self.tiles[:k]) for k in range(4)]
        self.n_row = up_to(sum(self.blocks), 8)
        self.spare = sum(self.tiles)
        self.n_column = up_to(self.spare + 1, 8)


def accumulate(k, places, g_ref, m_ref, r_ref, own_ref, out_ref, partial):
    h, n_blocks, tiles = places.halves[k], places.blocks[k], places.tiles[k]
    row_at, column_at = places.row_at[k], places.n_row + places.column_at[k]

    def step(i, sums):
        rows = pl.ds(pl.multiple_of(i * 8, 8), 8)
        sums = list(sums)
        by_row = None
        for j in range(tiles):
            at = (rows, pl.ds(j * LANES, LANES))
            grad = g_ref[at] + r_ref[at]
            own_ref[at] = momentum_decay * m_ref[at] + (1.0 - momentum_decay) * grad
            square = grad * grad
            sums[j] = sums[j] + square
            by_row = square if by_row is None else by_row + square
        partial[rows, :] = by_row
        return tuple(sums)

    zero = jnp.zeros((8, LANES), jnp.float32)
    sums = lax.fori_loop(0, h // 8, step, (zero,) * tiles, unroll=4)
    for j in range(tiles):
        out_ref[pl.ds(column_at + j, 1), :] = jnp.sum(sums[j], axis=0, keepdims=True)
    if n_blocks * LANES > h:
        partial[pl.ds(h, n_blocks * LANES - h), :] = jnp.zeros((n_blocks * LANES - h, LANES), jnp.float32)
    for b in range(n_blocks):
        turned = partial[pl.ds(b * LANES, LANES), :].T
        out_ref[pl.ds(row_at + b, 1), :] = jnp.sum(turned, axis=0, keepdims=True)


def own_halves(places, partials, momenta, received):
    first, later = ORDER[0], ORDER[1:]
    h, width = places.halves[first], places.widths[first]

    def kernel(*refs):
        me = lax.axis_index("rep")
        g_refs, m_refs, r_ref = refs[:4], refs[4:8], refs[8]
        held = dict(zip(later, zip(refs[9:12], refs[12:15])))
        own_ref, out_ref = refs[15:17]
        held[first] = refs[17:19]
        partial, sem = refs[19], refs[20]
        started = []
        for k in ORDER:
            at = pl.ds(pl.multiple_of(me * places.halves[k], 8), places.halves[k])
            for source, target in zip((g_refs[k].at[0, at], m_refs[k].at[at]), held[k]):
                started.append(pltpu.make_async_copy(source, target, sem.at[len(started)]))
                started[-1].start()
        out_ref[...] = jnp.zeros_like(out_ref)
        for item in started[:2]:
            item.wait()
        accumulate(first, places, *held[first], r_ref, own_ref, out_ref, partial)
        for item in started[2:]:
            item.wait()

    halves = [struct(places.halves[k], places.widths[k]) for k in later]
    out = call(
        kernel,
        [*partials, *momenta, received],
        [*halves, *halves, struct(h, width), struct(places.n_row + places.n_column, LANES)],
        [HBM] * 8 + [VMEM],
        [VMEM] * 8,
        [pltpu.VMEM((h, width), jnp.float32)] * 2
        + [pltpu.VMEM((places.blocks[first] * LANES, LANES), jnp.float32), pltpu.SemaphoreType.DMA((8,))],
        limit=(4 << 20) + 8 * h * width,
        cost=1 << 22,
    )
    return dict(zip(later, zip(out[:3], out[3:6]))), out[6], out[7]


def statistics(k, places, g, m, received, packed):
    h, width = g.shape

    def kernel(g_ref, m_ref, r_ref, packed_ref, own_ref, out_ref, partial):
        accumulate(k, places, g_ref, m_ref, r_ref, own_ref, out_ref, partial)

    return call(
        kernel,
        [g, m, received, packed],
        [struct(h, width), struct(*packed.shape)],
        [VMEM] * 4,
        [VMEM, VMEM],
        [pltpu.VMEM((places.blocks[k] * LANES, LANES), jnp.float32)],
        cost=1 << 20,
        aliases={3: 1},
    )


def spread_rows(root, factor, n_blocks):
    for b in range(n_blocks):
        wide = jnp.broadcast_to(root[b : b + 1, :], (LANES, LANES)).T
        factor[pl.ds(b * LANES, LANES), :] = wide


def shares(places, column_count, rows_old, row_parts, packed, own, after, early=()):
    n_parts = len(row_parts)

    def old_rows(k, ref, me):
        h, n = places.halves[k], places.blocks[k]
        whole, rest = divmod(h, LANES)
        everything = ref[...]
        first = everything[:n]
        if rest:
            turned = pltpu.roll(everything, LANES - rest, 1)
            low = lax.broadcasted_iota(jnp.int32, (1, LANES), 1) < LANES - rest
            steps = []
            for i in range(n):
                here = turned[whole + i : whole + i + 1]
                after = turned[whole + i + 1 : whole + i + 2] if i < n - 1 else here
                steps.append(jnp.where(low, here, after))
            second = jnp.concatenate(steps, axis=0)
            at = lax.broadcasted_iota(jnp.int32, (n, LANES), 0) * LANES + lax.broadcasted_iota(jnp.int32, (n, LANES), 1)
            return jnp.where(at < h, jnp.where(me == 0, first, second), 0.0)
        return jnp.where(me == 0, first, everything[n:])

    def kernel(*refs):
        rows_refs, packed_ref = refs[:4], refs[4]
        part_refs, own_refs = refs[5 : 5 + n_parts], refs[5 + n_parts : 9 + n_parts]
        rows_out, factor, out_ref = refs[-3:]
        lane = lax.broadcasted_iota(jnp.int32, (1, LANES), 1)
        total = packed_ref[pl.ds(0, places.n_row), :]
        for part in part_refs:
            total = total + part[...]
        me = lax.axis_index("rep")
        mass = jnp.zeros((1, LANES), jnp.float32)
        out_ref[pl.ds(0, places.n_column), :] = packed_ref[pl.ds(places.n_row, places.n_column), :]
        out_ref[pl.ds(2 * places.n_column - 8, 8), :] = jnp.zeros((8, LANES), jnp.float32)
        news = []
        for k in range(4):
            at = slice(places.row_at[k], places.row_at[k] + places.blocks[k])
            r = moment_decay * old_rows(k, rows_refs[k], me) + (1.0 - moment_decay) / column_count[k] * total[at, :]
            news.append(r)
            mass = jnp.where(lane == k, jnp.sum(r), mass)
            rows_out[pl.ds(places.row_at[k], places.blocks[k]), :] = r
        fill = places.n_row - sum(places.blocks)
        if fill:
            rows_out[pl.ds(sum(places.blocks), fill), :] = jnp.ones((fill, LANES), jnp.float32)
        spread_rows(lax.rsqrt(jnp.concatenate(news, axis=0)), factor, sum(places.blocks))
        for k, m_ref in enumerate(own_refs):
            first = places.row_at[k] * LANES

            def step(i, sums):
                sums = list(sums)
                by_row = factor[pl.ds(pl.multiple_of(first + i * 8, 8), 8), :]
                for j in range(places.tiles[k]):
                    v = m_ref[pl.ds(pl.multiple_of(i * 8, 8), 8), pl.ds(j * LANES, LANES)] * by_row
                    sums[j] = sums[j] + v * v
                return tuple(sums)

            zero = jnp.zeros((8, LANES), jnp.float32)
            sums = lax.fori_loop(0, places.halves[k] // 8, step, (zero,) * places.tiles[k], unroll=2)
            for j in range(places.tiles[k]):
                at = pl.ds(places.n_column + places.column_at[k] + j, 1)
                out_ref[at, :] = jnp.sum(sums[j], axis=0, keepdims=True)
        out_ref[pl.ds(places.n_column + places.spare, 1), :] = mass

    return call(
        kernel,
        [*rows_old, packed, *row_parts, *own, *after, *early],
        [struct(places.n_row, LANES), struct(sum(places.blocks) * LANES, LANES), struct(2 * places.n_column, LANES)],
        [VMEM] * (9 + n_parts) + [HBM] * len(after) + [VMEM] * len(early),
        [VMEM] * 3,
        cost=1 << 21,
    )


def columns(places, row_count, columns_old, total, other, after, early=()):
    def kernel(c0, c1, c2, c3, total_ref, other_ref, *rest):
        columns_out, out_ref = rest[-2:]
        old_refs = (c0, c1, c2, c3)
        lane = lax.broadcasted_iota(jnp.int32, (1, LANES), 1)
        both = total_ref[...] + other_ref[...]
        mass = jnp.zeros((1, LANES), jnp.float32)
        columns_out[pl.ds(places.n_column - 8, 8), :] = jnp.zeros((8, LANES), jnp.float32)
        row_mass = both[places.n_column + places.spare : places.n_column + places.spare + 1, :]
        for k in range(4):
            at = slice(places.column_at[k], places.column_at[k] + places.tiles[k])
            c = moment_decay * old_refs[k][...] + (1.0 - moment_decay) / row_count[k] * both[at, :]
            columns_out[pl.ds(places.column_at[k], places.tiles[k]), :] = c
            at = slice(places.n_column + at.start, places.n_column + at.stop)
            mass = jnp.where(lane == k, jnp.sum(both[at, :] / c), mass)
            mass = jnp.where(lane == 4 + k, jnp.sum(jnp.where(lane == k, row_mass, 0.0)), mass)
        out_ref[...] = jnp.broadcast_to(mass, (8, LANES))

    return call(
        kernel,
        [*columns_old, total, other, *after, *early],
        [struct(places.n_column, LANES), struct(8, LANES)],
        [VMEM] * 6 + [HBM] * len(after) + [VMEM] * len(early),
        [VMEM] * 2,
        cost=1 << 20,
    )


def write_own(own, shapes, after, early=()):
    def kernel(*refs):
        me = lax.axis_index("rep")
        pairs = []
        for k in range(4):
            h = refs[k].shape[0]
            pairs.append((refs[k], refs[5 + len(early) + k].at[pl.ds(pl.multiple_of(me * h, 8), h)]))
        copies(pairs, refs[-1])

    return call(
        kernel,
        [*own, after, *early],
        shapes,
        [VMEM] * (5 + len(early)),
        [HBM] * 4,
        [pltpu.SemaphoreType.DMA((4,))],
        cost=1 << 24,
    )


def write_back(places, back, momenta, rows_own, rows_other, columns_new):
    counts = [2 * h // LANES for h in places.halves]

    def kernel(*refs):
        me = lax.axis_index("rep")
        own_ref, other_ref, columns_ref = refs[8:11]
        outs, small, factor = refs[11:15], refs[15:23], refs[23]
        stages, sem = refs[24:32], refs[32]
        started = []

        def begin(source, target):
            started.append(pltpu.make_async_copy(source, target, sem.at[len(started)]))
            started[-1].start()

        for k in range(4):
            h = refs[k].shape[0]
            begin(refs[k], outs[k].at[pl.ds(pl.multiple_of((1 - me) * h, 8), h)])
        for k in range(4):
            h, n = places.halves[k], places.blocks[k]
            row_ref, column_ref = stages[k], stages[4 + k]
            column_ref[...] = columns_ref[pl.ds(places.column_at[k], places.tiles[k]), :]
            mine = own_ref[pl.ds(places.row_at[k], n), :]
            other = other_ref[pl.ds(places.row_at[k], n), :]
            first = jnp.where(me == 0, mine, other)
            second = jnp.where(me == 0, other, mine)
            whole, rest = divmod(h, LANES)
            if not rest:
                row_ref[pl.ds(0, n), :] = first
                row_ref[pl.ds(n, n), :] = second
            else:
                turned = pltpu.roll(second, rest, 1)
                low = lax.broadcasted_iota(jnp.int32, (1, LANES), 1) < rest
                row_ref[pl.ds(0, whole), :] = first[:whole]
                before = first[whole : whole + 1]
                for i in range(counts[k] - whole):
                    here = turned[i : i + 1]
                    row_ref[pl.ds(whole + i, 1), :] = jnp.where(low, before, here)
                    before = here
            begin(row_ref, small[k])
            begin(column_ref, small[4 + k])
        spread_rows(lax.rsqrt(other_ref[...]), factor, sum(places.blocks))
        for item in started:
            item.wait()

    sizes = counts + places.tiles
    out = call(
        kernel,
        [*back, *momenta, rows_own, rows_other, columns_new],
        [struct(*m.shape) for m in momenta]
        + [struct(n, LANES) for n in sizes]
        + [struct(sum(places.blocks) * LANES, LANES)],
        [VMEM] * 4 + [HBM] * 4 + [VMEM] * 3,
        [HBM] * 12 + [VMEM],
        [pltpu.VMEM((n, LANES), jnp.float32) for n in sizes] + [pltpu.SemaphoreType.DMA((12,))],
        cost=1 << 24,
        aliases={4 + k: k for k in range(4)},
    )
    return out[:4], out[4:8], out[8:12], out[12]


def write_weights(places, row_count, column_count, n_share, masses, factors, columns_new, own, back, weights, outs):
    n_parts = len(masses)

    def kernel(*refs):
        part_refs, refs = refs[:n_parts], refs[n_parts:]
        factor_refs, columns_ref = refs[:2], refs[2]
        own_refs, back_refs, w_refs, out_refs = (refs[3 + 4 * n : 7 + 4 * n] for n in range(4))
        stages, sem = refs[19:23], refs[23]
        me = lax.axis_index("rep")
        masses_all = sum((part[pl.ds(0, 1), :] for part in part_refs[1:]), part_refs[0][pl.ds(0, 1), :])
        lane = lax.broadcasted_iota(jnp.int32, (1, LANES), 1)

        def pick(n):
            return jnp.sum(jnp.where(lane == n, masses_all, 0.0), axis=1, keepdims=True)

        waits = []
        for k in range(4):
            h, tiles = places.halves[k], places.tiles[k]
            row_mean = pick(4 + k) / (n_share * row_count[k])
            spread = jnp.sqrt(pick(k) * row_mean / (row_count[k] * column_count[k]))
            scale = step_rate * jnp.sqrt(row_mean) / jnp.maximum(1.0, spread / clip_level)
            by_column = lax.rsqrt(columns_ref[pl.ds(places.column_at[k], tiles), :]) * scale
            wide = [jnp.broadcast_to(by_column[j : j + 1, :], (8, LANES)) for j in range(tiles)]
            chunk = h // PARTS if h % (8 * PARTS) == 0 else h
            first = places.row_at[k] * LANES
            for side, m_ref in enumerate((own_refs[k], back_refs[k])):
                which = me if side == 0 else 1 - me
                factor_ref = factor_refs[side]
                for begin in range(0, h, chunk):

                    def step(i, carry):
                        near = pl.multiple_of(begin + i * 8, 8)
                        far = pl.multiple_of(which * h + begin + i * 8, 8)
                        by_row = factor_ref[pl.ds(pl.multiple_of(first + begin + i * 8, 8), 8), :]
                        for j in range(tiles):
                            lanes = pl.ds(j * LANES, LANES)
                            change = m_ref[pl.ds(near, 8), lanes] * by_row * wide[j]
                            stages[k][pl.ds(far, 8), lanes] = w_refs[k][pl.ds(far, 8), lanes] - change
                        return carry

                    lax.fori_loop(0, chunk // 8, step, 0, unroll=2)
                    at = pl.ds(pl.multiple_of(which * h + begin, 8), chunk)
                    copy = pltpu.make_async_copy(stages[k].at[at], out_refs[k].at[at], sem.at[len(waits)])
                    copy.start()
                    waits.append(copy)
        for copy in waits:
            copy.wait()

    scratch = [pltpu.VMEM(w.shape, jnp.float32) for w in weights] + [pltpu.SemaphoreType.DMA((8 * PARTS,))]
    limit = sum(w.size * 4 for w in weights) + (4 << 20)
    return call(
        kernel,
        [*masses, *factors, columns_new, *own, *back, *weights],
        outs,
        [VMEM] * (n_parts + 15),
        [HBM] * 4,
        scratch,
        limit=limit,
        cost=1 << 22,
    )


def shifted(x, axis):
    n = lax.axis_size(axis)
    out = []
    for d in range(1, n):
        if n & (n - 1):
            pairs = [(i, (i + d) % n) for i in range(n)]
        else:
            pairs = [(i, i ^ d) for i in range(n)]
        out.append(lax.ppermute(x, axis, pairs))
    return out


def fast_body(*args):
    weights, momenta, partials, rows, columns_in = (args[k::5] for k in range(5))
    n_fs, n_tp = lax.axis_size("fs"), lax.axis_size("tp")
    heights = [item.shape[0] for item in weights]
    widths = [item.shape[1] for item in weights]
    row_count = [h * n_fs for h in heights]
    column_count = [w * n_tp for w in widths]
    places = Places(heights, widths)
    shapes = [struct(*w.shape) for w in weights]

    received = [None] * 4
    for group in (ORDER[:1], ORDER[1:]):
        for k, other in zip(group, other_halves([partials[k] for k in group])):
            received[k] = swap(other)
    rows_old = [item.reshape(-1, LANES) for item in rows]
    columns_old = [item.reshape(-1, LANES) for item in columns_in]
    own, back = [None] * 4, [None] * 4
    halves, own[ORDER[0]], packed = own_halves(places, partials, momenta, received[ORDER[0]])
    for k in ORDER[1:]:
        own[k], packed = statistics(k, places, *halves[k], received[k], packed)
    for k in ORDER:
        back[k] = swap(own[k])

    row_parts = shifted(packed[: places.n_row], "tp")
    rows_own, factor_own, local = shares(places, column_count, rows_old, row_parts, packed, own, (), weights)

    rows_other = swap(rows_own)
    total = sum(shifted(local, "fs"), local)
    momenta_next = write_own(own, shapes, local)
    columns_new, mass = columns(places, row_count, columns_old, total, swap(total), ())

    masses = [mass, *shifted(mass, "tp")]
    momenta_next, rows_new, columns_out, factor_other = write_back(
        places, back, momenta_next, rows_own, rows_other, columns_new
    )
    weights_next = write_weights(
        places, row_count, column_count, n_tp, masses, [factor_own, factor_other], columns_new, own, back, weights, shapes
    )
    out = []
    for k in range(4):
        out += [weights_next[k], momenta_next[k], rows_new[k].reshape(-1), columns_out[k].reshape(-1)]
    return tuple(out)


def half(x, which):
    size = x.shape[0] // 2
    return lax.dynamic_slice_in_dim(x, which * size, size, 0)


def join(own, other, me):
    first = me == 0
    return jnp.concatenate([jnp.where(first, own, other), jnp.where(first, other, own)], axis=0)


def cross_sums(row_part, column_part, me):
    n_fs, n_tp = lax.axis_size("fs"), lax.axis_size("tp")
    if n_fs != n_tp:
        return lax.psum(row_part, "tp"), lax.psum(column_part, "fs")
    length = max(row_part.size, column_part.size)

    def padded(x):
        return jnp.pad(x, (0, length - x.size))

    mine = jnp.where(me == 1, padded(row_part), padded(column_part))
    total = mine
    for shift in range(1, n_tp):
        pairs = []
        for f in range(n_fs):
            for t in range(n_tp):
                here = (f * n_tp + t) * 2
                pairs.append((here + 1, (f * n_tp + (t + shift) % n_tp) * 2 + 1))
                pairs.append((here, ((f + shift) % n_fs * n_tp + t) * 2))
        total = total + lax.ppermute(mine, EVERY, pairs)
    other = swap(total)
    rows = jnp.where(me == 1, total, other)[: row_part.size]
    columns = jnp.where(me == 1, other, total)[: column_part.size]
    return rows, columns


def plain_body(*args):
    weights, momenta, partials, rows, columns = (args[k::5] for k in range(5))
    me = lax.axis_index("rep")
    n_all = lax.axis_size(EVERY)
    partials = [item[0] for item in partials]
    heights = [item.shape[0] for item in weights]
    widths = [item.shape[1] for item in weights]
    row_count = [h * lax.axis_size("fs") for h in heights]
    column_count = [w * lax.axis_size("tp") for w in widths]

    received = [None] * 4
    for k in ORDER:
        received[k] = swap(half(partials[k], 1 - me))
    own = [None] * 4
    back = [None] * 4
    row_local = [None] * 4
    column_local = [None] * 4
    for k in ORDER:
        grad = half(partials[k], me) + received[k]
        own[k] = momentum_decay * half(momenta[k], me) + (1.0 - momentum_decay) * grad
        back[k] = swap(own[k])
        square = grad * grad
        placed = jnp.zeros((heights[k],), jnp.float32)
        row_local[k] = lax.dynamic_update_slice_in_dim(
            placed, jnp.sum(square, axis=1), me * (heights[k] // 2), 0
        )
        column_local[k] = jnp.sum(square, axis=0)

    local = jnp.concatenate(row_local + column_local)
    local = local + swap(local)
    n_rows = sum(heights)
    row_total, column_total = cross_sums(local[:n_rows], local[n_rows:], me)

    rows_next, columns_next = [], []
    at_row = at_column = 0
    for k in range(4):
        r = row_total[at_row : at_row + heights[k]]
        c = column_total[at_column : at_column + widths[k]]
        at_row += heights[k]
        at_column += widths[k]
        rows_next.append(moment_decay * rows[k] + (1.0 - moment_decay) * r / column_count[k])
        columns_next.append(moment_decay * columns[k] + (1.0 - moment_decay) * c / row_count[k])

    mass = []
    for k in range(4):
        m = own[k]
        mass.append(jnp.sum(m * m / half(rows_next[k], me)[:, None] / columns_next[k][None, :]))
    row_mass = [jnp.sum(half(rows_next[k], me)) for k in range(4)]
    scalars = jnp.stack(mass + row_mass)
    spread_out = jnp.broadcast_to(scalars[None], (n_all, 8))
    totals = jnp.sum(lax.all_to_all(spread_out, EVERY, 0, 0), axis=0)

    weights_next, momenta_next = [], []
    for k in range(4):
        row_mean = totals[4 + k] / (lax.axis_size("tp") * row_count[k])
        spread = jnp.sqrt(totals[k] * row_mean / (row_count[k] * column_count[k]))
        factor = jnp.maximum(1.0, spread / clip_level)
        scale = step_rate * jnp.sqrt(row_mean) / factor
        m = join(own[k], back[k], me)
        momenta_next.append(m)
        by_row = lax.rsqrt(rows_next[k]) * scale
        by_column = lax.rsqrt(columns_next[k])
        weights_next.append(weights[k] - m * by_row[:, None] * by_column[None, :])
    out = []
    for k in range(4):
        out += [weights_next[k], momenta_next[k], rows_next[k], columns_next[k]]
    return tuple(out)


def fits(args):
    small = max(lax.axis_size("fs"), lax.axis_size("tp")) <= 8
    return small and all(n % LANES == 0 for item in args[0::5] for n in item.shape)


def body(*args):
    return fast_body(*args) if fits(args) else plain_body(*args)


def solution(mesh):
    matrix, stacked = P("fs", "tp"), P("rep", "fs", "tp")

    return jax.shard_map(
        body,
        mesh=mesh,
        in_specs=(matrix, matrix, stacked, P("fs"), P("tp")) * 4,
        out_specs=(matrix, matrix, P("fs"), P("tp")) * 4,
        check_vma=False,
    )
```

```python
import jax
import jax.numpy as jnp
from jax import lax
from jax.experimental import pallas as pl
from jax.experimental.pallas import tpu as pltpu
from jax.sharding import PartitionSpec as P


momentum_decay = 0.9
moment_decay = 0.95
clip_level = 0.25
step_rate = 0.1

EVERY = ("fs", "tp", "rep")
SWAP = [(0, 1), (1, 0)]
ORDER = (2, 0, 1, 3)
LANES = 128
PARTS = 2
HBM = pl.BlockSpec(memory_space=pltpu.HBM)
VMEM = pl.BlockSpec(memory_space=pltpu.VMEM)


def up_to(n, unit):
    return (n + unit - 1) // unit * unit


def struct(*shape):
    return jax.ShapeDtypeStruct(shape, jnp.float32)


def call(kernel, ins, outs, spaces, out_spaces, scratch=(), limit=4 << 20, cost=0, aliases=None):
    ins = [pltpu.with_memory_space_constraint(x, spec.memory_space) for x, spec in zip(ins, spaces)]
    placed = [spec.memory_space(out.shape, out.dtype) for out, spec in zip(outs, out_spaces)]
    return pl.pallas_call(
        kernel,
        out_shape=placed,
        in_specs=spaces,
        out_specs=out_spaces,
        scratch_shapes=scratch,
        input_output_aliases=aliases or {},
        compiler_params=pltpu.CompilerParams(vmem_limit_bytes=limit),
        cost_estimate=pl.CostEstimate(flops=cost, bytes_accessed=0, transcendentals=0),
    )(*ins)


def swap(x):
    return lax.ppermute(x, "rep", SWAP)


def copies(pairs, sem):
    started = [pltpu.make_async_copy(a, b, sem.at[n]) for n, (a, b) in enumerate(pairs)]
    for item in started:
        item.start()
    for item in started:
        item.wait()


def other_halves(arrays):
    n = len(arrays)

    def kernel(*refs):
        me = lax.axis_index("rep")
        pairs = []
        for source, target in zip(refs[:n], refs[n : 2 * n]):
            h = target.shape[0]
            pairs.append((source.at[0, pl.ds(pl.multiple_of((1 - me) * h, 8), h)], target))
        copies(pairs, refs[-1])

    outs = [struct(g.shape[1] // 2, g.shape[2]) for g in arrays]
    return call(kernel, arrays, outs, [HBM] * n, [VMEM] * n, [pltpu.SemaphoreType.DMA((n,))], cost=1 << 21)


class Places:
    def __init__(self, heights, widths):
        self.halves = [h // 2 for h in heights]
        self.widths = widths
        self.blocks = [up_to(h, LANES) // LANES for h in self.halves]
        self.tiles = [w // LANES for w in widths]
        self.row_at = [sum(self.blocks[:k]) for k in range(4)]
        self.column_at = [sum(self.tiles[:k]) for k in range(4)]
        self.n_row = up_to(sum(self.blocks), 8)
        self.spare = sum(self.tiles)
        self.n_column = up_to(self.spare + 1, 8)


def accumulate(k, places, g_ref, m_ref, r_ref, own_ref, out_ref, partial):
    h, n_blocks, tiles = places.halves[k], places.blocks[k], places.tiles[k]
    row_at, column_at = places.row_at[k], places.n_row + places.column_at[k]

    def step(i, sums):
        rows = pl.ds(pl.multiple_of(i * 8, 8), 8)
        sums = list(sums)
        by_row = None
        for j in range(tiles):
            at = (rows, pl.ds(j * LANES, LANES))
            grad = g_ref[at] + r_ref[at]
            own_ref[at] = momentum_decay * m_ref[at] + (1.0 - momentum_decay) * grad
            square = grad * grad
            sums[j] = sums[j] + square
            by_row = square if by_row is None else by_row + square
        partial[rows, :] = by_row
        return tuple(sums)

    zero = jnp.zeros((8, LANES), jnp.float32)
    sums = lax.fori_loop(0, h // 8, step, (zero,) * tiles, unroll=4)
    for j in range(tiles):
        out_ref[pl.ds(column_at + j, 1), :] = jnp.sum(sums[j], axis=0, keepdims=True)
    if n_blocks * LANES > h:
        partial[pl.ds(h, n_blocks * LANES - h), :] = jnp.zeros((n_blocks * LANES - h, LANES), jnp.float32)
    for b in range(n_blocks):
        turned = partial[pl.ds(b * LANES, LANES), :].T
        out_ref[pl.ds(row_at + b, 1), :] = jnp.sum(turned, axis=0, keepdims=True)


def own_halves(places, partials, momenta, received):
    first, later = ORDER[0], ORDER[1:]
    h, width = places.halves[first], places.widths[first]

    def kernel(*refs):
        me = lax.axis_index("rep")
        g_refs, m_refs, r_ref = refs[:4], refs[4:8], refs[8]
        held = dict(zip(later, zip(refs[9:12], refs[12:15])))
        own_ref, out_ref = refs[15:17]
        held[first] = refs[17:19]
        partial, sem = refs[19], refs[20]
        started = []
        for k in ORDER:
            at = pl.ds(pl.multiple_of(me * places.halves[k], 8), places.halves[k])
            for source, target in zip((g_refs[k].at[0, at], m_refs[k].at[at]), held[k]):
                started.append(pltpu.make_async_copy(source, target, sem.at[len(started)]))
                started[-1].start()
        out_ref[...] = jnp.zeros_like(out_ref)
        for item in started[:2]:
            item.wait()
        accumulate(first, places, *held[first], r_ref, own_ref, out_ref, partial)
        for item in started[2:]:
            item.wait()

    halves = [struct(places.halves[k], places.widths[k]) for k in later]
    out = call(
        kernel,
        [*partials, *momenta, received],
        [*halves, *halves, struct(h, width), struct(places.n_row + places.n_column, LANES)],
        [HBM] * 8 + [VMEM],
        [VMEM] * 8,
        [pltpu.VMEM((h, width), jnp.float32)] * 2
        + [pltpu.VMEM((places.blocks[first] * LANES, LANES), jnp.float32), pltpu.SemaphoreType.DMA((8,))],
        limit=(4 << 20) + 8 * h * width,
        cost=1 << 22,
    )
    return dict(zip(later, zip(out[:3], out[3:6]))), out[6], out[7]


def statistics(k, places, g, m, received, packed):
    h, width = g.shape

    def kernel(g_ref, m_ref, r_ref, packed_ref, own_ref, out_ref, partial):
        accumulate(k, places, g_ref, m_ref, r_ref, own_ref, out_ref, partial)

    return call(
        kernel,
        [g, m, received, packed],
        [struct(h, width), struct(*packed.shape)],
        [VMEM] * 4,
        [VMEM, VMEM],
        [pltpu.VMEM((places.blocks[k] * LANES, LANES), jnp.float32)],
        cost=1 << 20,
        aliases={3: 1},
    )


def spread_rows(root, factor, n_blocks):
    for b in range(n_blocks):
        wide = jnp.broadcast_to(root[b : b + 1, :], (LANES, LANES)).T
        factor[pl.ds(b * LANES, LANES), :] = wide


def shares(places, column_count, rows_old, row_parts, packed, own, after, early=()):
    n_parts = len(row_parts)

    def old_rows(k, ref, me):
        h, n = places.halves[k], places.blocks[k]
        whole, rest = divmod(h, LANES)
        everything = ref[...]
        first = everything[:n]
        if rest:
            turned = pltpu.roll(everything, LANES - rest, 1)
            low = lax.broadcasted_iota(jnp.int32, (1, LANES), 1) < LANES - rest
            steps = []
            for i in range(n):
                here = turned[whole + i : whole + i + 1]
                after = turned[whole + i + 1 : whole + i + 2] if i < n - 1 else here
                steps.append(jnp.where(low, here, after))
            second = jnp.concatenate(steps, axis=0)
            at = lax.broadcasted_iota(jnp.int32, (n, LANES), 0) * LANES + lax.broadcasted_iota(jnp.int32, (n, LANES), 1)
            return jnp.where(at < h, jnp.where(me == 0, first, second), 0.0)
        return jnp.where(me == 0, first, everything[n:])

    def kernel(*refs):
        rows_refs, packed_ref = refs[:4], refs[4]
        part_refs, own_refs = refs[5 : 5 + n_parts], refs[5 + n_parts : 9 + n_parts]
        rows_out, factor, out_ref = refs[-3:]
        lane = lax.broadcasted_iota(jnp.int32, (1, LANES), 1)
        total = packed_ref[pl.ds(0, places.n_row), :]
        for part in part_refs:
            total = total + part[...]
        me = lax.axis_index("rep")
        mass = jnp.zeros((1, LANES), jnp.float32)
        out_ref[pl.ds(0, places.n_column), :] = packed_ref[pl.ds(places.n_row, places.n_column), :]
        out_ref[pl.ds(2 * places.n_column - 8, 8), :] = jnp.zeros((8, LANES), jnp.float32)
        news = []
        for k in range(4):
            at = slice(places.row_at[k], places.row_at[k] + places.blocks[k])
            r = moment_decay * old_rows(k, rows_refs[k], me) + (1.0 - moment_decay) / column_count[k] * total[at, :]
            news.append(r)
            mass = jnp.where(lane == k, jnp.sum(r), mass)
            rows_out[pl.ds(places.row_at[k], places.blocks[k]), :] = r
        fill = places.n_row - sum(places.blocks)
        if fill:
            rows_out[pl.ds(sum(places.blocks), fill), :] = jnp.ones((fill, LANES), jnp.float32)
        spread_rows(lax.rsqrt(jnp.concatenate(news, axis=0)), factor, sum(places.blocks))
        for k, m_ref in enumerate(own_refs):
            first = places.row_at[k] * LANES

            def step(i, sums):
                sums = list(sums)
                by_row = factor[pl.ds(pl.multiple_of(first + i * 8, 8), 8), :]
                for j in range(places.tiles[k]):
                    v = m_ref[pl.ds(pl.multiple_of(i * 8, 8), 8), pl.ds(j * LANES, LANES)] * by_row
                    sums[j] = sums[j] + v * v
                return tuple(sums)

            zero = jnp.zeros((8, LANES), jnp.float32)
            sums = lax.fori_loop(0, places.halves[k] // 8, step, (zero,) * places.tiles[k], unroll=8)
            for j in range(places.tiles[k]):
                at = pl.ds(places.n_column + places.column_at[k] + j, 1)
                out_ref[at, :] = jnp.sum(sums[j], axis=0, keepdims=True)
        out_ref[pl.ds(places.n_column + places.spare, 1), :] = mass

    return call(
        kernel,
        [*rows_old, packed, *row_parts, *own, *after, *early],
        [struct(places.n_row, LANES), struct(sum(places.blocks) * LANES, LANES), struct(2 * places.n_column, LANES)],
        [VMEM] * (9 + n_parts) + [HBM] * len(after) + [VMEM] * len(early),
        [VMEM] * 3,
        cost=1 << 21,
    )


def columns(places, row_count, columns_old, total, other, after, early=()):
    def kernel(c0, c1, c2, c3, total_ref, other_ref, *rest):
        columns_out, out_ref = rest[-2:]
        old_refs = (c0, c1, c2, c3)
        lane = lax.broadcasted_iota(jnp.int32, (1, LANES), 1)
        both = total_ref[...] + other_ref[...]
        mass = jnp.zeros((1, LANES), jnp.float32)
        columns_out[pl.ds(places.n_column - 8, 8), :] = jnp.zeros((8, LANES), jnp.float32)
        row_mass = both[places.n_column + places.spare : places.n_column + places.spare + 1, :]
        for k in range(4):
            at = slice(places.column_at[k], places.column_at[k] + places.tiles[k])
            c = moment_decay * old_refs[k][...] + (1.0 - moment_decay) / row_count[k] * both[at, :]
            columns_out[pl.ds(places.column_at[k], places.tiles[k]), :] = c
            at = slice(places.n_column + at.start, places.n_column + at.stop)
            mass = jnp.where(lane == k, jnp.sum(both[at, :] / c), mass)
            mass = jnp.where(lane == 4 + k, jnp.sum(jnp.where(lane == k, row_mass, 0.0)), mass)
        out_ref[...] = jnp.broadcast_to(mass, (8, LANES))

    return call(
        kernel,
        [*columns_old, total, other, *after, *early],
        [struct(places.n_column, LANES), struct(8, LANES)],
        [VMEM] * 6 + [HBM] * len(after) + [VMEM] * len(early),
        [VMEM] * 2,
        cost=1 << 20,
    )


def write_own(own, shapes, after, early=()):
    def kernel(*refs):
        me = lax.axis_index("rep")
        pairs = []
        for k in range(4):
            h = refs[k].shape[0]
            pairs.append((refs[k], refs[5 + len(early) + k].at[pl.ds(pl.multiple_of(me * h, 8), h)]))
        copies(pairs, refs[-1])

    return call(
        kernel,
        [*own, after, *early],
        shapes,
        [VMEM] * (5 + len(early)),
        [HBM] * 4,
        [pltpu.SemaphoreType.DMA((4,))],
        cost=1 << 24,
    )


def write_back(places, back, momenta, rows_own, rows_other, columns_new):
    counts = [2 * h // LANES for h in places.halves]

    def kernel(*refs):
        me = lax.axis_index("rep")
        own_ref, other_ref, columns_ref = refs[8:11]
        outs, small, factor = refs[11:15], refs[15:23], refs[23]
        stages, sem = refs[24:32], refs[32]
        started = []

        def begin(source, target):
            started.append(pltpu.make_async_copy(source, target, sem.at[len(started)]))
            started[-1].start()

        for k in range(4):
            h = refs[k].shape[0]
            begin(refs[k], outs[k].at[pl.ds(pl.multiple_of((1 - me) * h, 8), h)])
        for k in range(4):
            h, n = places.halves[k], places.blocks[k]
            row_ref, column_ref = stages[k], stages[4 + k]
            column_ref[...] = columns_ref[pl.ds(places.column_at[k], places.tiles[k]), :]
            mine = own_ref[pl.ds(places.row_at[k], n), :]
            other = other_ref[pl.ds(places.row_at[k], n), :]
            first = jnp.where(me == 0, mine, other)
            second = jnp.where(me == 0, other, mine)
            whole, rest = divmod(h, LANES)
            if not rest:
                row_ref[pl.ds(0, n), :] = first
                row_ref[pl.ds(n, n), :] = second
            else:
                turned = pltpu.roll(second, rest, 1)
                low = lax.broadcasted_iota(jnp.int32, (1, LANES), 1) < rest
                row_ref[pl.ds(0, whole), :] = first[:whole]
                before = first[whole : whole + 1]
                for i in range(counts[k] - whole):
                    here = turned[i : i + 1]
                    row_ref[pl.ds(whole + i, 1), :] = jnp.where(low, before, here)
                    before = here
            begin(row_ref, small[k])
            begin(column_ref, small[4 + k])
        spread_rows(lax.rsqrt(other_ref[...]), factor, sum(places.blocks))
        for item in started:
            item.wait()

    sizes = counts + places.tiles
    out = call(
        kernel,
        [*back, *momenta, rows_own, rows_other, columns_new],
        [struct(*m.shape) for m in momenta]
        + [struct(n, LANES) for n in sizes]
        + [struct(sum(places.blocks) * LANES, LANES)],
        [VMEM] * 4 + [HBM] * 4 + [VMEM] * 3,
        [HBM] * 12 + [VMEM],
        [pltpu.VMEM((n, LANES), jnp.float32) for n in sizes] + [pltpu.SemaphoreType.DMA((12,))],
        cost=1 << 24,
        aliases={4 + k: k for k in range(4)},
    )
    return out[:4], out[4:8], out[8:12], out[12]


def write_weights(places, row_count, column_count, n_share, masses, factors, columns_new, own, back, weights, outs):
    n_parts = len(masses)

    def kernel(*refs):
        part_refs, refs = refs[:n_parts], refs[n_parts:]
        factor_refs, columns_ref = refs[:2], refs[2]
        own_refs, back_refs, w_refs, out_refs = (refs[3 + 4 * n : 7 + 4 * n] for n in range(4))
        stages, sem = refs[19:23], refs[23]
        me = lax.axis_index("rep")
        masses_all = sum((part[pl.ds(0, 1), :] for part in part_refs[1:]), part_refs[0][pl.ds(0, 1), :])
        lane = lax.broadcasted_iota(jnp.int32, (1, LANES), 1)

        def pick(n):
            return jnp.sum(jnp.where(lane == n, masses_all, 0.0), axis=1, keepdims=True)

        waits = []
        for k in range(4):
            h, tiles = places.halves[k], places.tiles[k]
            row_mean = pick(4 + k) / (n_share * row_count[k])
            spread = jnp.sqrt(pick(k) * row_mean / (row_count[k] * column_count[k]))
            scale = step_rate * jnp.sqrt(row_mean) / jnp.maximum(1.0, spread / clip_level)
            by_column = lax.rsqrt(columns_ref[pl.ds(places.column_at[k], tiles), :]) * scale
            wide = [jnp.broadcast_to(by_column[j : j + 1, :], (8, LANES)) for j in range(tiles)]
            chunk = h // PARTS if h % (8 * PARTS) == 0 else h
            first = places.row_at[k] * LANES
            for side, m_ref in enumerate((own_refs[k], back_refs[k])):
                which = me if side == 0 else 1 - me
                factor_ref = factor_refs[side]
                for begin in range(0, h, chunk):

                    def step(i, carry):
                        near = pl.multiple_of(begin + i * 8, 8)
                        far = pl.multiple_of(which * h + begin + i * 8, 8)
                        by_row = factor_ref[pl.ds(pl.multiple_of(first + begin + i * 8, 8), 8), :]
                        for j in range(tiles):
                            lanes = pl.ds(j * LANES, LANES)
                            change = m_ref[pl.ds(near, 8), lanes] * by_row * wide[j]
                            stages[k][pl.ds(far, 8), lanes] = w_refs[k][pl.ds(far, 8), lanes] - change
                        return carry

                    lax.fori_loop(0, chunk // 8, step, 0, unroll=4)
                    at = pl.ds(pl.multiple_of(which * h + begin, 8), chunk)
                    copy = pltpu.make_async_copy(stages[k].at[at], out_refs[k].at[at], sem.at[len(waits)])
                    copy.start()
                    waits.append(copy)
        for copy in waits:
            copy.wait()

    scratch = [pltpu.VMEM(w.shape, jnp.float32) for w in weights] + [pltpu.SemaphoreType.DMA((8 * PARTS,))]
    limit = sum(w.size * 4 for w in weights) + (4 << 20)
    return call(
        kernel,
        [*masses, *factors, columns_new, *own, *back, *weights],
        outs,
        [VMEM] * (n_parts + 15),
        [HBM] * 4,
        scratch,
        limit=limit,
        cost=1 << 22,
    )


def shifted(x, axis):
    n = lax.axis_size(axis)
    out = []
    for d in range(1, n):
        if n & (n - 1):
            pairs = [(i, (i + d) % n) for i in range(n)]
        else:
            pairs = [(i, i ^ d) for i in range(n)]
        out.append(lax.ppermute(x, axis, pairs))
    return out


def fast_body(*args):
    weights, momenta, partials, rows, columns_in = (args[k::5] for k in range(5))
    n_fs, n_tp = lax.axis_size("fs"), lax.axis_size("tp")
    heights = [item.shape[0] for item in weights]
    widths = [item.shape[1] for item in weights]
    row_count = [h * n_fs for h in heights]
    column_count = [w * n_tp for w in widths]
    places = Places(heights, widths)
    shapes = [struct(*w.shape) for w in weights]

    received = [None] * 4
    for group in (ORDER[:1], ORDER[1:]):
        for k, other in zip(group, other_halves([partials[k] for k in group])):
            received[k] = swap(other)
    rows_old = [item.reshape(-1, LANES) for item in rows]
    columns_old = [item.reshape(-1, LANES) for item in columns_in]
    own, back = [None] * 4, [None] * 4
    halves, own[ORDER[0]], packed = own_halves(places, partials, momenta, received[ORDER[0]])
    for k in ORDER[1:]:
        own[k], packed = statistics(k, places, *halves[k], received[k], packed)
    for k in ORDER:
        back[k] = swap(own[k])

    row_parts = shifted(packed[: places.n_row], "tp")
    rows_own, factor_own, local = shares(places, column_count, rows_old, row_parts, packed, own, (), weights)

    rows_other = swap(rows_own)
    total = sum(shifted(local, "fs"), local)
    momenta_next = write_own(own, shapes, local)
    columns_new, mass = columns(places, row_count, columns_old, total, swap(total), ())

    masses = [mass, *shifted(mass, "tp")]
    momenta_next, rows_new, columns_out, factor_other = write_back(
        places, back, momenta_next, rows_own, rows_other, columns_new
    )
    weights_next = write_weights(
        places, row_count, column_count, n_tp, masses, [factor_own, factor_other], columns_new, own, back, weights, shapes
    )
    out = []
    for k in range(4):
        out += [weights_next[k], momenta_next[k], rows_new[k].reshape(-1), columns_out[k].reshape(-1)]
    return tuple(out)


def half(x, which):
    size = x.shape[0] // 2
    return lax.dynamic_slice_in_dim(x, which * size, size, 0)


def join(own, other, me):
    first = me == 0
    return jnp.concatenate([jnp.where(first, own, other), jnp.where(first, other, own)], axis=0)


def cross_sums(row_part, column_part, me):
    n_fs, n_tp = lax.axis_size("fs"), lax.axis_size("tp")
    if n_fs != n_tp:
        return lax.psum(row_part, "tp"), lax.psum(column_part, "fs")
    length = max(row_part.size, column_part.size)

    def padded(x):
        return jnp.pad(x, (0, length - x.size))

    mine = jnp.where(me == 1, padded(row_part), padded(column_part))
    total = mine
    for shift in range(1, n_tp):
        pairs = []
        for f in range(n_fs):
            for t in range(n_tp):
                here = (f * n_tp + t) * 2
                pairs.append((here + 1, (f * n_tp + (t + shift) % n_tp) * 2 + 1))
                pairs.append((here, ((f + shift) % n_fs * n_tp + t) * 2))
        total = total + lax.ppermute(mine, EVERY, pairs)
    other = swap(total)
    rows = jnp.where(me == 1, total, other)[: row_part.size]
    columns = jnp.where(me == 1, other, total)[: column_part.size]
    return rows, columns


def plain_body(*args):
    weights, momenta, partials, rows, columns = (args[k::5] for k in range(5))
    me = lax.axis_index("rep")
    n_all = lax.axis_size(EVERY)
    partials = [item[0] for item in partials]
    heights = [item.shape[0] for item in weights]
    widths = [item.shape[1] for item in weights]
    row_count = [h * lax.axis_size("fs") for h in heights]
    column_count = [w * lax.axis_size("tp") for w in widths]

    received = [None] * 4
    for k in ORDER:
        received[k] = swap(half(partials[k], 1 - me))
    own = [None] * 4
    back = [None] * 4
    row_local = [None] * 4
    column_local = [None] * 4
    for k in ORDER:
        grad = half(partials[k], me) + received[k]
        own[k] = momentum_decay * half(momenta[k], me) + (1.0 - momentum_decay) * grad
        back[k] = swap(own[k])
        square = grad * grad
        placed = jnp.zeros((heights[k],), jnp.float32)
        row_local[k] = lax.dynamic_update_slice_in_dim(
            placed, jnp.sum(square, axis=1), me * (heights[k] // 2), 0
        )
        column_local[k] = jnp.sum(square, axis=0)

    local = jnp.concatenate(row_local + column_local)
    local = local + swap(local)
    n_rows = sum(heights)
    row_total, column_total = cross_sums(local[:n_rows], local[n_rows:], me)

    rows_next, columns_next = [], []
    at_row = at_column = 0
    for k in range(4):
        r = row_total[at_row : at_row + heights[k]]
        c = column_total[at_column : at_column + widths[k]]
        at_row += heights[k]
        at_column += widths[k]
        rows_next.append(moment_decay * rows[k] + (1.0 - moment_decay) * r / column_count[k])
        columns_next.append(moment_decay * columns[k] + (1.0 - moment_decay) * c / row_count[k])

    mass = []
    for k in range(4):
        m = own[k]
        mass.append(jnp.sum(m * m / half(rows_next[k], me)[:, None] / columns_next[k][None, :]))
    row_mass = [jnp.sum(half(rows_next[k], me)) for k in range(4)]
    scalars = jnp.stack(mass + row_mass)
    spread_out = jnp.broadcast_to(scalars[None], (n_all, 8))
    totals = jnp.sum(lax.all_to_all(spread_out, EVERY, 0, 0), axis=0)

    weights_next, momenta_next = [], []
    for k in range(4):
        row_mean = totals[4 + k] / (lax.axis_size("tp") * row_count[k])
        spread = jnp.sqrt(totals[k] * row_mean / (row_count[k] * column_count[k]))
        factor = jnp.maximum(1.0, spread / clip_level)
        scale = step_rate * jnp.sqrt(row_mean) / factor
        m = join(own[k], back[k], me)
        momenta_next.append(m)
        by_row = lax.rsqrt(rows_next[k]) * scale
        by_column = lax.rsqrt(columns_next[k])
        weights_next.append(weights[k] - m * by_row[:, None] * by_column[None, :])
    out = []
    for k in range(4):
        out += [weights_next[k], momenta_next[k], rows_next[k], columns_next[k]]
    return tuple(out)


def fits(args):
    small = max(lax.axis_size("fs"), lax.axis_size("tp")) <= 8
    return small and all(n % LANES == 0 for item in args[0::5] for n in item.shape)


def body(*args):
    return fast_body(*args) if fits(args) else plain_body(*args)


def solution(mesh):
    matrix, stacked = P("fs", "tp"), P("rep", "fs", "tp")

    return jax.shard_map(
        body,
        mesh=mesh,
        in_specs=(matrix, matrix, stacked, P("fs"), P("tp")) * 4,
        out_specs=(matrix, matrix, P("fs"), P("tp")) * 4,
        check_vma=False,
    )
```
